512 devices in a mesh: grp: 2 (over y), sp: 32 (over z), tp: 8 (over x, core).
Axes of the slice: x: 4, y: 2, z: 32, core: 2. Of those that a mesh axis runs over, the one named last changes fastest.
The devices are a block of a 4x8x32 slice.
Arguments:
- starting_stream: bfloat16 [24576, 2048], P(('grp', 'sp'), 'tp'), parts along dimension 0, may hold values from -45 to 45
- multiplier_matrix: bfloat16 [2, 2048, 2048], P(None, 'sp', 'tp'), may hold values from -0.125 to 0.125
- memory_path_matrix: bfloat16 [2, 2048, 2048], P(None, 'sp', 'tp'), may hold values from -0.125 to 0.125
- filter_coefficients: bfloat16 [2, 4, 2048], P(None, None, 'tp'), may hold values from -3 to 3
- memory_valve_matrix: bfloat16 [2, 8, 256, 256], P(None, 'tp'), may hold values from -0.375 to 0.375
- entry_valve_matrix: bfloat16 [2, 8, 256, 256], P(None, 'tp'), may hold values from -0.375 to 0.375
- forgetting_parameters: float32 [2, 2048], P(None, 'tp'), may hold values from 3 to 15
- timestep_forgetting_multiplier: float32 [24576], P(('grp', 'sp')), parts along dimension 0, may hold values from 0.5 to 2
- spike_extra: float32 [24576, 2048], P(('grp', 'sp'), 'tp'), parts along dimension 0, may hold values from -0.7 to 0
- exit_projector_matrix: bfloat16 [2, 2048, 2048], P(None, 'tp', 'sp'), may hold values from -0.125 to 0.125
- prelude_rms_gains: float32 [2, 2048], replicated, may hold values from 0.1 to 1.9
- finishing_rms_gains: float32 [2048], P('tp'), may hold values from 0.1 to 1.9
Outputs:
- result: bfloat16 [24576, 2048], P(('grp', 'sp'), 'tp'), parts along dimension 0
The draws below stay inside these ranges and needn't reach their ends.
There are 2 independent parts, one for each index of `grp`. The reference program is written for one: setup_inputs(seed, part) draws one part's arguments, and reference() takes and returns one part's arrays. A program takes and returns all parts, laid end to end along the dimension named above; an argument that names none is the same for every part. Nothing has to cross between parts.
All inputs are finite; a program needn't handle non-finite values.
Results may differ from the reference program's by a relative error of at most 0.015.
Values may be sent and summed in bfloat16 or wider, within the bound.
A program may use at most 64 MiB of HBM per device.

```python
import math
import jax
import jax.numpy as jnp
from jax import lax

D = 2048
W = 2048
BLOCK_W = 256
BLOCKS = 8
CONV = 4
LAYERS = 2
TOK_DEV = 384
TOKENS = 12288
N_TP = 8


def draw_starting_stream(key, part):
    keys = jax.random.split(key, 3)
    columns = jnp.arange(D, dtype=jnp.float32)
    col_scale = jnp.exp(math.log(4.0) * columns / D) * jax.random.uniform(keys[1], (D,), jnp.float32, 0.7, 1.4)
    row_scale = jnp.exp(jax.random.uniform(keys[2], (TOKENS, 1), jnp.float32, math.log(0.5), math.log(2.0)))
    base = jnp.clip(jax.random.normal(keys[0], (TOKENS, D), jnp.float32), -4.0, 4.0)
    return (base * col_scale[None, :] * row_scale).astype(jnp.bfloat16)


def draw_forgetting_parameters(key, part):
    keys = jax.random.split(key, 3)
    share_fast = 0.5
    fast = jax.random.bernoulli(keys[0], share_fast, (LAYERS, W))
    fast_rate = jnp.exp(jax.random.uniform(keys[1], (LAYERS, W), jnp.float32, math.log(0.01), math.log(0.03)))
    slow_rate = jnp.exp(jax.random.uniform(keys[2], (LAYERS, W), jnp.float32, math.log(0.1), math.log(0.5))) / (4.0 * TOKENS)
    rate = jnp.where(fast, fast_rate, slow_rate)
    return -jnp.log(jnp.expm1(rate))


def draw_timestep_forgetting_multiplier(key, part):
    counted = TOKENS // TOK_DEV
    values = jnp.exp(jax.random.uniform(key, (counted,), jnp.float32, math.log(0.5), math.log(2.0)))
    return jnp.repeat(values, TOK_DEV, total_repeat_length=TOKENS)


def draw_spike_extra(key, part):
    keys = jax.random.split(key, 2)
    spots = jax.random.randint(keys[0], (4,), 0, TOKENS)
    places = jnp.arange(TOKENS, dtype=jnp.int32)
    struck = jnp.any(places[:, None] == spots[None, :], axis=1)
    depth = jnp.log(jax.random.uniform(keys[1], (TOKENS, W), jnp.float32, 0.5, 0.8))
    return jnp.where(struck[:, None], depth, 0.0)


def levels(own_key, dims, shards, least, high):
    factor_of, own = 1.0, jax.random.fold_in(own_key, 6)
    for axis_at, shards_of in shards:
        draws = jnp.exp(jax.random.uniform(jax.random.fold_in(own, axis_at), (shards_of,), jnp.float32, least / len(shards), high / len(shards)))
        factor_of = factor_of * jnp.repeat(draws, dims[axis_at] // shards_of).reshape([-1 if axis == axis_at else 1 for axis in range(len(dims))])
    return factor_of


def gaussian(stream_key, shape, scale, reach, shards=(), held_as=jnp.bfloat16):
    level = levels(stream_key, shape, shards, -0.22, 0.18) if shards else 1.0
    array = jax.random.normal(stream_key, shape, jnp.float32) * scale * level
    return jnp.minimum(jnp.maximum(array, -reach), reach).astype(held_as)


def setup_inputs(seed: int = 0, part: int = 0) -> dict:
    seeds = jax.random.split(jax.random.key(seed), 13)
    part_keys = jax.random.split(jax.random.fold_in(seeds[12], part), 13)
    return {
        "starting_stream": draw_starting_stream(jax.random.fold_in(jax.random.fold_in(seeds[12], part), 71), part),
        "multiplier_matrix": gaussian(seeds[1], (LAYERS, D, W), D ** -0.5, 0.125, ((1, 32), (2, 8))),
        "memory_path_matrix": gaussian(seeds[2], (LAYERS, D, W), D ** -0.5, 0.125, ((1, 32), (2, 8))),
        "filter_coefficients": gaussian(seeds[3], (LAYERS, CONV, W), CONV ** -0.5, 3.0, ((2, 8),)),
        "memory_valve_matrix": gaussian(seeds[4], (LAYERS, BLOCKS, BLOCK_W, BLOCK_W), BLOCK_W ** -0.5, 0.375, ((1, 8),)),
        "entry_valve_matrix": gaussian(seeds[5], (LAYERS, BLOCKS, BLOCK_W, BLOCK_W), BLOCK_W ** -0.5, 0.375, ((1, 8),)),
        "forgetting_parameters": draw_forgetting_parameters(jax.random.fold_in(seeds[12], 71), part),
        "timestep_forgetting_multiplier": draw_timestep_forgetting_multiplier(jax.random.fold_in(jax.random.fold_in(seeds[12], part), 71), part),
        "spike_extra": draw_spike_extra(jax.random.fold_in(jax.random.fold_in(seeds[12], part), 71), part),
        "exit_projector_matrix": gaussian(seeds[9], (LAYERS, W, D), W ** -0.5, 0.125, ((1, 8), (2, 32))),
        "prelude_rms_gains": jnp.clip(1.0 + 0.18 * jax.random.normal(seeds[10], (LAYERS, D), jnp.float32), 0.1, 1.9),
        "finishing_rms_gains": jnp.clip(1.0 + 0.18 * jax.random.normal(seeds[11], (D,), jnp.float32), 0.1, 1.9),
    }


EPSILON = 1e-06
SQUASH_POWER = 8.0

def norm_rows(values, gain):
    mean_square = lax.optimization_barrier(jnp.mean(values * values, axis=-1, keepdims=True))
    return values * lax.rsqrt(mean_square + EPSILON) * gain

def combine_pairs(earlier, later):
    return (earlier[0] * later[0], later[0] * earlier[1] + later[1])

def reference(starting_stream, multiplier_matrix, memory_path_matrix, filter_coefficients, memory_valve_matrix, entry_valve_matrix, forgetting_parameters, timestep_forgetting_multiplier, spike_extra, exit_projector_matrix, prelude_rms_gains, finishing_rms_gains):
    stream = starting_stream
    full_width = memory_path_matrix.shape[2]
    per_block = full_width // N_TP
    for tier_number in range(LAYERS):
        floats = stream.astype(jnp.float32)
        normed = norm_rows(floats, prelude_rms_gains[tier_number]).astype(jnp.bfloat16)
        branch = jnp.dot(normed, multiplier_matrix[tier_number], preferred_element_type=jnp.float32).astype(jnp.bfloat16)
        recurrent = jnp.dot(normed, memory_path_matrix[tier_number], preferred_element_type=jnp.float32).astype(jnp.bfloat16)
        padded = jnp.concatenate([jnp.zeros((CONV - 1, full_width), jnp.bfloat16), recurrent], axis=0)
        conv_sum = jnp.zeros((TOKENS, full_width), jnp.float32)
        for offset in range(CONV):
            conv_sum = conv_sum + padded[offset:offset + TOKENS].astype(jnp.float32) * filter_coefficients[tier_number, offset].astype(jnp.float32)
        convolved = conv_sum.astype(jnp.bfloat16)
        blocks = convolved.astype(jnp.float32).reshape(TOKENS, BLOCKS, BLOCK_W)
        memory_valve_amount = jax.nn.sigmoid(jnp.einsum('tnc,ncd->tnd', blocks, memory_valve_matrix[tier_number].astype(jnp.float32)).reshape(TOKENS, full_width))
        inject = jax.nn.sigmoid(jnp.einsum('tnc,ncd->tnd', blocks, entry_valve_matrix[tier_number].astype(jnp.float32)).reshape(TOKENS, full_width))
        logarithmic_persistence = -SQUASH_POWER * memory_valve_amount * jax.nn.softplus(-forgetting_parameters[tier_number])[None, :] * timestep_forgetting_multiplier[:, None] + spike_extra
        keep_rate = jnp.exp(logarithmic_persistence)
        driven = inject * convolved.astype(jnp.float32) * jnp.sqrt(-jnp.expm1(2.0 * logarithmic_persistence))
        state_seq = lax.associative_scan(combine_pairs, (keep_rate, driven), axis=0)[1]
        mixed_in = (jax.nn.gelu(branch.astype(jnp.float32)) * state_seq).astype(jnp.bfloat16)
        mixed_sum = jnp.zeros((TOKENS, D), jnp.float32)
        for block_no in range(N_TP):
            lower = block_no * per_block
            product = jnp.dot(mixed_in[:, lower:lower + per_block], exit_projector_matrix[tier_number, lower:lower + per_block], preferred_element_type=jnp.float32)
            mixed_sum = mixed_sum + lax.optimization_barrier(product.astype(jnp.bfloat16)).astype(jnp.float32)
        stream = (floats + mixed_sum).astype(jnp.bfloat16)
    return norm_rows(stream.astype(jnp.float32), finishing_rms_gains).astype(jnp.bfloat16)
```

```python
import functools

import jax
import jax.numpy as jnp
from jax import lax
from jax.experimental import pallas as pl
from jax.experimental.pallas import tpu as pltpu
from jax.sharding import PartitionSpec as P

EPSILON = 1e-06
SQUASH_POWER = 8.0
SEGS = 8
MESH = pl.DeviceIdType.MESH
F32 = jnp.float32
BF16 = jnp.bfloat16
NT = (((1,), (1,)), ((), ()))


def one_minus_exp(y):
    series = 1.0 + y * (1.0 / 8.0)
    for n in (7, 6, 5, 4, 3, 2):
        series = 1.0 + y * (1.0 / n) * series
    return jnp.where(y > -0.35, -y * series, 1.0 - jnp.exp(y))


def softplus(v):
    u = jnp.exp(-jnp.abs(v))
    s = u / (2.0 + u)
    s2 = s * s
    acc = jnp.full_like(s, 1.0 / 17.0)
    for n in (15, 13, 11, 9, 7, 5, 3, 1):
        acc = acc * s2 + 1.0 / n
    return jnp.maximum(v, 0.0) + 2.0 * s * acc


def gelu(x):
    inner = 0.7978845608028654 * (x + 0.044715 * (x * x * x))
    return 0.5 * x * (1.0 + jnp.tanh(inner))


def kernel(
    n_sp,
    n_x,
    x_hbm,
    wm_hbm,
    wp_hbm,
    ex_hbm,
    rv_hbm,
    iv_hbm,
    spike_hbm,
    filt_ref,
    forget_ref,
    tm_ref,
    gain_ref,
    fin_ref,
    out_ref,
    xin,
    exin,
    rv,
    iv,
    spike_in,
    spk,
    tmc,
    xf,
    w,
    nrm,
    rec,
    br,
    kp,
    dr,
    pp,
    own32,
    psnd,
    prcv,
    rsnd,
    rrcv,
    hsnd,
    hrcv,
    csnd,
    crcv,
    nsnd,
    nrcv,
    lsem,
    z_s,
    z_r,
    ag_s,
    ag_r,
    ad_s,
    ad_r,
    rs_s,
    rs_r,
    rd_s,
    rd_r,
    h_s,
    h_r,
    c_s,
    c_r,
    n_s,
    n_r,
):
    layers = wm_hbm.shape[0]
    rows, cols = x_hbm.shape
    half = rows // 2
    steps = rows // SEGS
    chunk = wm_hbm.shape[1]
    n_tp = 2 * n_x
    z = lax.axis_index("sp")
    me = lax.axis_index("tp")
    x = me // 2
    c = lax.rem(me, 2)
    other = 1 - c
    z_up, z_dn = lax.rem(z + 1, n_sp), lax.rem(z + n_sp - 1, n_sp)
    x_rt, x_lf, x_far = lax.rem(x + 1, n_x), lax.rem(x + n_x - 1, n_x), lax.rem(x + 2, n_x)
    mate = {"tp": 2 * x + other}
    right, left = {"tp": 2 * x_rt + c}, {"tp": 2 * x_lf + c}
    up, down = {"sp": z_up}, {"sp": z_dn}

    def remote(src, dst, ssem, rsem, dev):
        return pltpu.make_async_remote_copy(
            src_ref=src, dst_ref=dst, send_sem=ssem, recv_sem=rsem, device_id=dev, device_id_type=MESH
        )

    own_rows = pl.ds(pl.multiple_of(z * chunk, chunk), chunk)
    local = [
        pltpu.make_async_copy(x_hbm, xin, lsem.at[0]),
        pltpu.make_async_copy(ex_hbm, exin, lsem.at[1]),
        pltpu.make_async_copy(rv_hbm, rv, lsem.at[2]),
        pltpu.make_async_copy(iv_hbm, iv, lsem.at[3]),
        pltpu.make_async_copy(spike_hbm, spike_in, lsem.at[4]),
    ]
    for l in range(layers):
        local.append(pltpu.make_async_copy(wp_hbm.at[l], w.at[l, 0, own_rows, :], lsem.at[5 + 2 * l]))
        local.append(pltpu.make_async_copy(wm_hbm.at[l], w.at[l, 1, own_rows, :], lsem.at[6 + 2 * l]))
    for copy in local:
        copy.start()

    barrier = pltpu.get_barrier_semaphore()
    for dev in (up, down):
        pl.semaphore_signal(barrier, inc=1, device_id=dev, device_id_type=MESH)
    for k in range(1, n_tp):
        pl.semaphore_signal(
            barrier, inc=1, device_id={"tp": lax.rem(me + k, n_tp)}, device_id_type=MESH
        )
    pl.semaphore_wait(barrier, n_tp + 1)

    last_up, last_dn = n_sp // 2, n_sp - 1 - n_sp // 2

    def z_copy(l, m, d, s):
        src = lax.rem(z - s + n_sp, n_sp) if d == 0 else lax.rem(z + s, n_sp)
        ref = w.at[l, m, pl.ds(pl.multiple_of(src * chunk, chunk), chunk), :]
        return remote(ref, ref, z_s.at[l, m, d, s], z_r.at[l, m, d, s], up if d == 0 else down)

    def z_land(l, m, d, s):
        src = lax.rem(z - s - 1 + n_sp, n_sp) if d == 0 else lax.rem(z + s + 1, n_sp)
        ref = w.at[l, m, pl.ds(pl.multiple_of(src * chunk, chunk), chunk), :]
        return remote(ref, ref, z_s.at[l, m, d, s], z_r.at[l, m, d, s], up if d == 0 else down)

    def ring_start(l, m):
        z_copy(l, m, 0, 0).start()
        z_copy(l, m, 1, 0).start()

    def ring_steps(l, first, last):
        both = min(last, last_dn - 1)

        def one(s, _):
            for m in range(3):
                for d in range(2):
                    z_land(l, m, d, s).wait_recv()
                    z_copy(l, m, d, s + 1).start()
            return 0

        if both > first:
            lax.fori_loop(first, both, one, 0)
        for s in range(max(first, both), last):
            for m in range(3):
                if s < last_up:
                    z_land(l, m, 0, s).wait_recv()
                    if s + 1 < last_up:
                        z_copy(l, m, 0, s + 1).start()
                if s < last_dn:
                    z_land(l, m, 1, s).wait_recv()
                    if s + 1 < last_dn:
                        z_copy(l, m, 1, s + 1).start()

    for i in (5, 6, 1):
        local[i].wait()
    ring_start(0, 0)
    ring_start(0, 1)
    for l in range(layers):
        w[l, 2, own_rows, :] = exin[l].astype(F32).T.astype(BF16)
    ring_start(0, 2)

    row_p = lax.broadcasted_iota(jnp.int32, (rows, rows), 0)
    row_r = lax.broadcasted_iota(jnp.int32, (rows, rows), 1)
    onehot = row_r == (row_p & (SEGS - 1)) * steps + (row_p >> 3)
    local[0].wait()
    xf[0, me] = jnp.dot(onehot.astype(BF16), xin[...], preferred_element_type=F32).astype(BF16)

    top, bottom = pl.ds(0, half), pl.ds(half, half)

    def ag_copy(l, i):
        block, part, dev = (
            (2 * x + c, top, right),
            (2 * x + c, bottom, right),
            (2 * x_lf + c, top, right),
            (2 * x + c, bottom, left),
            (2 * x + c, top, left),
            (2 * x_rt + c, bottom, left),
        )[i]
        ref = xf.at[l, block, part, :]
        return remote(ref, ref, ag_s.at[l, i], ag_r.at[l, i], dev)

    def ag_land(l, i):
        block, part = (
            (2 * x_lf + c, top),
            (2 * x_lf + c, bottom),
            (2 * x_far + c, top),
            (2 * x_rt + c, bottom),
            (2 * x_rt + c, top),
            (2 * x_far + c, bottom),
        )[i]
        ref = xf.at[l, block, part, :]
        return remote(ref, ref, ag_s.at[l, i], ag_r.at[l, i], right)

    def ad_copy(l, i):
        ref = xf.at[l, 2 * (x, x_lf, x_rt, x_far)[i] + c]
        return remote(ref, ref, ad_s.at[l, i], ad_r.at[l, i], mate)

    def ad_land(l, i):
        ref = xf.at[l, 2 * (x, x_lf, x_rt, x_far)[i] + other]
        return remote(ref, ref, ad_s.at[l, i], ad_r.at[l, i], mate)

    def ag_start(l):
        for i in (0, 3, 1, 4):
            ag_copy(l, i).start()
        ad_copy(l, 0).start()

    def ag_forward(l):
        ag_land(l, 0).wait_recv()
        ag_copy(l, 2).start()
        ag_land(l, 3).wait_recv()
        ag_copy(l, 5).start()

    def ag_near(l):
        ag_land(l, 1).wait_recv()
        ad_copy(l, 1).start()
        ag_land(l, 4).wait_recv()
        ad_copy(l, 2).start()

    def ag_far(l):
        ag_land(l, 2).wait_recv()
        ag_land(l, 5).wait_recv()
        ad_copy(l, 3).start()
        for i in range(4):
            ad_land(l, i).wait_recv()

    def normalize(l):
        size = 32

        def one(i, _):
            part = pl.ds(pl.multiple_of(i * size, size), size)
            total = jnp.zeros((size, cols), F32)
            for b in range(n_tp):
                v = xf[l, b, part, :].astype(F32)
                total = total + v * v
            inv = lax.rsqrt(jnp.sum(total, axis=1, keepdims=True) / (n_tp * cols) + EPSILON)
            for b in range(n_tp):
                g = gain_ref[l : l + 1, b * cols : (b + 1) * cols]
                nrm[part, b * cols : (b + 1) * cols] = (xf[l, b, part, :].astype(F32) * inv * g).astype(BF16)
            return 0

        lax.fori_loop(0, rows // size, one, 0)

    def recurrent(l):
        rec[pl.ds(24, rows), :] = (
            jnp.dot(nrm[...], w[l, 0], preferred_element_type=F32).astype(BF16).astype(F32)
        )
        for j in range(3):
            at = 24 + rows - 24 + 8 * j + 7
            hsnd[l, j : j + 1, :] = rec[at : at + 1, :]
        h_copy = remote(hsnd.at[l], hrcv.at[l], h_s.at[l], h_r.at[l], up)

        @pl.when(z < n_sp - 1)
        def _():
            h_copy.start()

        @pl.when(z == 0)
        def _():
            hrcv[l] = jnp.zeros((8, cols), F32)

        @pl.when(z > 0)
        def _():
            h_copy.wait_recv()

        first = lax.broadcasted_iota(jnp.int32, (8, cols), 0) == 0
        for j in range(3):
            tail = rec[rows + 8 * j : rows + 8 * j + 8, :]
            rec[8 * j : 8 * j + 8, :] = jnp.where(
                first, jnp.broadcast_to(hrcv[l, j : j + 1, :], (8, cols)), pltpu.roll(tail, 1, 0)
            )

        @pl.when(z < n_sp - 1)
        def _():
            h_copy.wait_send()

    def gates(l):
        size = 64
        rate = softplus(-forget_ref[l : l + 1, :]) * -SQUASH_POWER
        f = filt_ref[l].astype(F32)

        def one(i, _):
            base = pl.multiple_of(i * size, size)
            conv = jnp.zeros((size, cols), F32)
            for k in range(4):
                conv = conv + rec[pl.ds(pl.multiple_of(base + 8 * k, 8), size), :] * f[k : k + 1, :]
            conv = conv.astype(BF16)
            reset = jax.nn.sigmoid(jnp.dot(conv, rv[l, 0], preferred_element_type=F32))
            inject = jax.nn.sigmoid(jnp.dot(conv, iv[l, 0], preferred_element_type=F32))
            part = pl.ds(base, size)
            tmb = jnp.concatenate([tmc[part, :]] * (cols // 128), axis=1)
            log_keep = reset * rate * tmb + spk[part, :]
            kp[part, :] = jnp.exp(log_keep)
            dr[part, :] = inject * conv.astype(F32) * jnp.sqrt(one_minus_exp(2.0 * log_keep))
            return 0

        lax.fori_loop(0, rows // size, one, 0)

    def scan(l):
        def one(i, carry):
            s, p = carry
            part = pl.ds(pl.multiple_of(i * SEGS, SEGS), SEGS)
            k = kp[part, :]
            s = k * s + dr[part, :]
            p = p * k
            dr[part, :] = s
            pp[part, :] = p
            return s, p

        s, p = lax.fori_loop(
            0, steps, one, (jnp.zeros((SEGS, cols), F32), jnp.ones((SEGS, cols), F32)), unroll=8
        )
        state, prod = jnp.zeros((1, cols), F32), jnp.ones((1, cols), F32)
        states, prods = [], []
        for j in range(SEGS):
            states.append(state)
            prods.append(prod)
            state = p[j : j + 1] * state + s[j : j + 1]
            prod = prod * p[j : j + 1]
        csnd[l, 0:1, :] = prod
        csnd[l, 1:2, :] = state
        return jnp.concatenate(states, axis=0), jnp.concatenate(prods, axis=0)

    def c_copy(l, target):
        return remote(csnd.at[l], crcv.at[l, z], c_s.at[l, target], c_r.at[l, z], {"sp": target})

    def carry_send(l):
        def one(n, _):
            for k in (n_sp // 2 - n, n_sp // 2 + 1 + n):
                target = z + k

                @pl.when(target < n_sp)
                def _():
                    c_copy(l, target).start()

            return 0

        lax.fori_loop(0, n_sp // 2, one, 0)

    def carry_wait(l):
        def one(n, carry):
            state, prod = carry
            j = z - 1 - n
            remote(csnd.at[l], crcv.at[l, j], c_s.at[l, j], c_r.at[l, j], {"sp": j}).wait_recv()
            state = state + prod * crcv[l, j, 1:2, :]
            prod = prod * crcv[l, j, 0:1, :]
            return state, prod

        return lax.fori_loop(0, z, one, (jnp.zeros((1, cols), F32), jnp.ones((1, cols), F32)))[0]

    def carry_drain(l):
        def one(target, _):
            c_copy(l, target).wait_send()
            return 0

        lax.fori_loop(z + 1, n_sp, one, 0)

    def branch(l):
        br[...] = gelu(jnp.dot(nrm[...], w[l, 1], preferred_element_type=F32).astype(BF16).astype(F32))

    def mix(carry):
        def one(i, _):
            part = pl.ds(pl.multiple_of(i * SEGS, SEGS), SEGS)
            br[part, :] = br[part, :] * (dr[part, :] + pp[part, :] * carry)
            return 0

        lax.fori_loop(0, steps, one, 0, unroll=8)

    def product(l, mixed, block):
        e = w[l, 2, pl.ds(pl.multiple_of(block * cols, cols), cols), :]
        return lax.dot_general(mixed, e, NT, preferred_element_type=F32)

    order = (x_far, x_rt, x_lf, x)

    def rd(l, i):
        return remote(psnd.at[i], prcv.at[l, i], rd_s.at[l, i], rd_r.at[l, i], mate)

    def rs(l, i):
        return remote(rsnd.at[i], rrcv.at[l, i], rs_s.at[l, i], rs_r.at[l, i], right if i < 3 else left)

    def rs_products(l):
        mixed = br[...].astype(BF16)
        for i in range(4):
            psnd[i] = product(l, mixed, 2 * order[i] + other).astype(BF16)
            rd(l, i).start()
        for i in range(4):
            own32[i] = product(l, mixed, 2 * order[i] + c)

    def pair(l, i, part):
        return own32[i, part, :] + prcv[l, i, part, :].astype(F32)

    def rs_first(l):
        rd(l, 0).wait_recv()
        rsnd[0] = pair(l, 0, top).astype(BF16)
        rs(l, 0).start()
        rsnd[3] = pair(l, 0, bottom).astype(BF16)
        rs(l, 3).start()
        rd(l, 1).wait_recv()
        rsnd[1] = pair(l, 1, bottom).astype(BF16)
        rs(l, 1).start()
        rd(l, 2).wait_recv()
        rsnd[4] = pair(l, 2, top).astype(BF16)
        rs(l, 4).start()

    def rs_second(l):
        rs(l, 0).wait_recv()
        rsnd[2] = (pair(l, 1, top) + rrcv[l, 0].astype(F32)).astype(BF16)
        rs(l, 2).start()
        rs(l, 3).wait_recv()
        rsnd[5] = (pair(l, 2, bottom) + rrcv[l, 3].astype(F32)).astype(BF16)
        rs(l, 5).start()

    def rs_last(l):
        rd(l, 3).wait_recv()
        parts = []
        for i in (1, 4, 2, 5):
            rs(l, i).wait_recv()
        for part, (a, b) in ((top, (2, 4)), (bottom, (1, 5))):
            total = pair(l, 3, part) + rrcv[l, a].astype(F32) + rrcv[l, b].astype(F32)
            parts.append((xf[l, me, part, :].astype(F32) + total).astype(BF16))
        for i in range(4):
            rd(l, i).wait_send()
        for i in range(6):
            rs(l, i).wait_send()
        return parts

    ag_start(0)
    ring_steps(0, 0, 2)
    ag_forward(0)
    ring_steps(0, 2, 4)
    ag_near(0)
    ring_steps(0, 4, 6)
    ag_far(0)
    tm_b = jnp.broadcast_to(tm_ref[...], (rows, rows))
    tmc[...] = jnp.broadcast_to(
        jnp.sum(jnp.where(onehot, tm_b, 0.0), axis=1, keepdims=True), tmc.shape
    )
    ring_steps(0, 6, 7)
    local[4].wait()
    spk[...] = jnp.dot(
        onehot.astype(F32), spike_in[...], preferred_element_type=F32, precision=lax.Precision.HIGHEST
    )
    ring_steps(0, 7, 8)
    normalize(0)
    ring_steps(0, 8, last_up)
    for i in (2, 3):
        local[i].wait()
    for l in range(1, layers):
        local[5 + 2 * l].wait()
        local[6 + 2 * l].wait()
        for m in range(3):
            ring_start(l, m)

    parts = None
    for l in range(layers):
        more = l + 1 < layers
        if l > 0:
            ag_start(l)
            ag_forward(l)
            ring_steps(l, 12, 13)
            ag_near(l)
            ring_steps(l, 13, 14)
            ag_far(l)
            normalize(l)
            ring_steps(l, 14, last_up)
        recurrent(l)
        gates(l)
        seg_state, seg_prod = scan(l)
        carry_send(l)
        branch(l)
        if more:
            ring_steps(l + 1, 0, 5)
        carry = carry_wait(l)
        mix(seg_state + seg_prod * carry)
        carry_drain(l)
        rs_products(l)
        rs_first(l)
        if more:
            ring_steps(l + 1, 5, 7)
        rs_second(l)
        if more:
            ring_steps(l + 1, 7, 9)
        parts = rs_last(l)
        if more:
            xf[l + 1, me, top, :] = parts[0]
            xf[l + 1, me, bottom, :] = parts[1]
            ring_steps(l + 1, 9, 12)

    final = jnp.concatenate(parts, axis=0).astype(F32)
    squares = jnp.sum(final * final, axis=1, keepdims=True)
    wide = jnp.transpose(jnp.broadcast_to(squares, (rows, 128)))
    nsnd[...] = wide[0:8, :]

    def n_copy(k):
        return remote(nsnd, nrcv.at[me], n_s.at[k], n_r.at[k], {"tp": lax.rem(me + k, n_tp)})

    for k in range(1, n_tp):
        n_copy(k).start()
    total = nsnd[...]
    for k in range(1, n_tp):
        n_copy(k).wait_recv()
    for k in range(1, n_tp):
        total = total + nrcv[lax.rem(me + k, n_tp)]
    inv = lax.rsqrt(total / (n_tp * cols) + EPSILON)
    inv = jnp.transpose(jnp.broadcast_to(inv[0:1, :], (128, rows)))
    inv = jnp.concatenate([inv] * (cols // 128), axis=1)
    result = (final * inv * fin_ref[...]).astype(BF16)
    back = row_p == (row_r & (SEGS - 1)) * steps + (row_r >> 3)
    out_ref[...] = jnp.dot(back.astype(BF16), result, preferred_element_type=F32).astype(BF16)

    for k in range(1, n_tp):
        n_copy(k).wait_send()
    for l in range(layers):
        for i in range(6):
            ag_copy(l, i).wait_send()
        for i in range(4):
            ad_copy(l, i).wait_send()
        for m in range(3):
            for d, last in ((0, last_up), (1, last_dn)):

                def one(s, _, l=l, m=m, d=d):
                    z_copy(l, m, d, s).wait_send()
                    return 0

                lax.fori_loop(0, last, one, 0)


def on_device(
    n_sp,
    n_tp,
    starting_stream,
    multiplier_matrix,
    memory_path_matrix,
    filter_coefficients,
    memory_valve_matrix,
    entry_valve_matrix,
    forgetting_parameters,
    timestep_forgetting_multiplier,
    spike_extra,
    exit_projector_matrix,
    prelude_rms_gains,
    finishing_rms_gains,
):
    rows, cols = starting_stream.shape
    layers, chunk, width = memory_path_matrix.shape
    half = rows // 2
    full = n_sp * chunk
    n_x = n_tp // 2
    hbm = pl.BlockSpec(memory_space=pl.ANY)
    vmem = pl.BlockSpec(memory_space=pltpu.VMEM)
    dma = pltpu.SemaphoreType.DMA
    scratch = [
        pltpu.VMEM((rows, cols), BF16),
        pltpu.VMEM(exit_projector_matrix.shape, BF16),
        pltpu.VMEM(memory_valve_matrix.shape, BF16),
        pltpu.VMEM(entry_valve_matrix.shape, BF16),
        pltpu.VMEM((rows, cols), F32),
        pltpu.VMEM((rows, cols), F32),
        pltpu.VMEM((rows, 128), F32),
        pltpu.VMEM((layers, n_tp, rows, cols), BF16),
        pltpu.VMEM((layers, 3, full, cols), BF16),
        pltpu.VMEM((rows, full), BF16),
        pltpu.VMEM((rows + 24, cols), F32),
        pltpu.VMEM((rows, cols), F32),
        pltpu.VMEM((rows, cols), F32),
        pltpu.VMEM((rows, cols), F32),
        pltpu.VMEM((rows, cols), F32),
        pltpu.VMEM((4, rows, cols), F32),
        pltpu.VMEM((4, rows, cols), BF16),
        pltpu.VMEM((layers, 4, rows, cols), BF16),
        pltpu.VMEM((6, half, cols), BF16),
        pltpu.VMEM((layers, 6, half, cols), BF16),
        pltpu.VMEM((layers, 8, cols), F32),
        pltpu.VMEM((layers, 8, cols), F32),
        pltpu.VMEM((layers, 2, cols), F32),
        pltpu.VMEM((layers, n_sp, 2, cols), F32),
        pltpu.VMEM((8, rows), F32),
        pltpu.VMEM((n_tp, 8, rows), F32),
        dma((9,)),
        dma((layers, 3, 2, n_sp // 2)),
        dma((layers, 3, 2, n_sp // 2)),
        dma((layers, 6)),
        dma((layers, 6)),
        dma((layers, 4)),
        dma((layers, 4)),
        dma((layers, 6)),
        dma((layers, 6)),
        dma((layers, 4)),
        dma((layers, 4)),
        dma((layers,)),
        dma((layers,)),
        dma((layers, n_sp)),
        dma((layers, n_sp)),
        dma((n_tp,)),
        dma((n_tp,)),
    ]
    return pl.pallas_call(
        functools.partial(kernel, n_sp, n_x),
        out_shape=jax.ShapeDtypeStruct((rows, cols), BF16),
        in_specs=[hbm] * 7 + [vmem] * 5,
        out_specs=vmem,
        scratch_shapes=scratch,
        compiler_params=pltpu.CompilerParams(
            collective_id=0, has_side_effects=True, vmem_limit_bytes=48 << 20
        ),
        name="layers",
    )(
        starting_stream,
        multiplier_matrix,
        memory_path_matrix,
        exit_projector_matrix,
        memory_valve_matrix,
        entry_valve_matrix,
        spike_extra,
        filter_coefficients,
        forgetting_parameters,
        timestep_forgetting_multiplier.reshape(1, rows),
        prelude_rms_gains,
        finishing_rms_gains.reshape(1, cols),
    )


def solution(mesh):
    return jax.shard_map(
        functools.partial(on_device, mesh.shape["sp"], mesh.shape["tp"]),
        mesh=mesh,
        in_specs=(
            P(("grp", "sp"), "tp"),
            P(None, "sp", "tp"),
            P(None, "sp", "tp"),
            P(None, None, "tp"),
            P(None, "tp", None, None),
            P(None, "tp", None, None),
            P(None, "tp"),
            P(("grp", "sp")),
            P(("grp", "sp"), "tp"),
            P(None, "tp", "sp"),
            P(),
            P("tp"),
        ),
        out_specs=P(("grp", "sp"), "tp"),
        check_vma=False,
    )
```
